32 devices in a mesh: grp: 2 (over y), ra: 4 (over z), cb: 4 (over x, core).
Axes of the slice: x: 2, y: 2, z: 4, core: 2. Of those that a mesh axis runs over, the one named last changes fastest.
Arguments:
- tokens: bfloat16 [2048, 4096], P('grp', 'ra'), parts along dimension 0, may hold values from -20 to 20
- norm_gain: float32 [2, 4096], P(None, 'ra'), may hold values from 0.1 to 1.9
- up_weight: float32 [2, 4096, 16384], P(None, 'ra', 'cb'), may hold values from -0.125 to 0.125
- up_scale: float32 [2, 16384], P(None, 'cb'), may hold values from 0.1 to 1.9
- down_weight: float32 [2, 16384, 4096], P(None, 'cb', 'ra'), may hold values from -0.046875 to 0.046875
- down_scale: float32 [2, 4096], P(None, 'ra'), may hold values from 0.1 to 1.9
Outputs:
- mixed: bfloat16 [2048, 4096], P('grp', 'ra'), parts along dimension 0
The draws below stay inside these ranges and needn't reach their ends.
There are 2 independent parts, one for each index of `grp`. The reference program is written for one: setup_inputs(seed, part) draws one part's arguments, and reference() takes and returns one part's arrays. A program takes and returns all parts, laid end to end along the dimension named above; an argument that names none is the same for every part. Nothing has to cross between parts.
All inputs are finite; a program needn't handle non-finite values.
Results may differ from the reference program's by a relative error of at most 0.023.
Values may be sent and summed in bfloat16 or wider, within the bound.
A program may use at most 192 MiB of HBM per device.

```python
import math
import jax
import jax.numpy as jnp
from jax import lax

D = 4096
FF = 16384
LAYERS = 2
TOKENS = 1024


def draw_tokens(key, part):
    first = jax.random.fold_in(key, 11)
    second = jax.random.fold_in(key, 23)
    groups = D // 128
    column_scale = jnp.exp(jax.random.uniform(second, (groups,), jnp.float32, math.log(0.3), math.log(3.0)))
    column_scale = jnp.repeat(column_scale, D // groups)
    values = jnp.clip(jax.random.normal(first, (TOKENS, D), jnp.float32), -6.0, 6.0)
    return jnp.clip(values * column_scale[None, :], -20.0, 20.0).astype(jnp.bfloat16)


def strengthened(array, key, source, target, parts, factor):
    def block_of(dim):
        return (jnp.arange(array.shape[dim]) // (array.shape[dim] // parts)).reshape((-1,) + (1,) * (array.ndim - 1 - dim))

    near = jax.random.permutation(key, parts)[block_of(target)]
    other_side = (block_of(target) + parts // 2) % parts
    return jnp.where((block_of(source) == near) | (block_of(source) == other_side), factor * array, array)


def block_levels(key, shape, shards, least, largest):
    def one(dim, shards_of):
        heights = jax.random.uniform(jax.random.fold_in(jax.random.fold_in(key, 6), dim), (shards_of,), jnp.float32, least / len(shards), largest / len(shards))
        return jnp.repeat(jnp.exp(heights), shape[dim] // shards_of).reshape((-1,) + (1,) * (len(shape) - dim - 1))

    level = one(*shards[0])
    for cut in shards[1:]:
        level = level * one(*cut)
    return level


def gaussian(stream_key, dims, spread, most, pieces=(), kind=jnp.bfloat16):
    entries = jax.random.normal(stream_key, dims, jnp.float32) * spread
    if len(pieces) > 0:
        entries = block_levels(stream_key, dims, pieces, -0.22, 0.18) * entries
    return jnp.clip(entries, min=-most, max=most).astype(kind)


def noise_with(own_key, shape, spread, bound, pieces, heavy, dtype=jnp.bfloat16):
    array = spread * jax.random.normal(own_key, shape, jnp.float32)
    if pieces:
        array = array * block_levels(own_key, shape, pieces, -0.22, 0.18)
    return jnp.clip(strengthened(array, jax.random.fold_in(own_key, 3), *heavy), -bound, bound).astype(dtype)


def setup_inputs(seed: int = 0, part: int = 0) -> dict:
    seeds = jax.random.split(jax.random.key(seed), 7)
    part_splits = jax.random.split(jax.random.fold_in(seeds[6], part), 7)
    tokens = draw_tokens(jax.random.fold_in(jax.random.fold_in(seeds[6], part), 71), part)
    norm_gain = jnp.clip(1.0 + 0.18 * jax.random.normal(seeds[1], (LAYERS, D), jnp.float32), 0.1, 1.9)
    up_weight = noise_with(seeds[2], (LAYERS, D, FF), D ** -0.5, 0.125, ((1, 4), (2, 4)), (1, 2, 4, 2.0), jnp.float32)
    up_scale = jnp.clip(1.0 + 0.18 * jax.random.normal(seeds[3], (LAYERS, FF), jnp.float32), 0.1, 1.9)
    down_weight = gaussian(seeds[4], (LAYERS, FF, D), FF ** -0.5, 0.046875, ((1, 4), (2, 4)), jnp.float32)
    down_scale = jnp.clip(1.0 + 0.18 * jax.random.normal(seeds[5], (LAYERS, D), jnp.float32), 0.1, 1.9)
    return dict(tokens=tokens, norm_gain=norm_gain, up_weight=up_weight, up_scale=up_scale, down_weight=down_weight, down_scale=down_scale)


epsilon = 1e-06
residual_keep = 0.5

def reference(tokens, norm_gain, up_weight, up_scale, down_weight, down_scale):
    current = tokens
    for sublayer in range(LAYERS):
        widened = current.astype(jnp.float32)
        mean_square = lax.optimization_barrier(jnp.mean(widened * widened, axis=1, keepdims=True))
        scaled = (widened * norm_gain[sublayer]).astype(jnp.bfloat16)
        upward = jnp.dot(scaled, up_weight[sublayer].astype(jnp.bfloat16), preferred_element_type=jnp.float32)
        active = jnp.maximum(upward * lax.rsqrt(mean_square + epsilon) * up_scale[sublayer], 0.0)
        hidden = (active * active).astype(jnp.bfloat16)
        downward = jnp.dot(hidden, down_weight[sublayer].astype(jnp.bfloat16), preferred_element_type=jnp.float32)
        current = (residual_keep * widened + downward * down_scale[sublayer]).astype(jnp.bfloat16)
    return current
```

```python
import jax
import jax.numpy as jnp
from jax import lax
from jax.sharding import PartitionSpec as P

D = 4096


epsilon = 1e-06
residual_keep = 0.5


f32, bf16 = jnp.float32, jnp.bfloat16


def dot(a, b):
    return jnp.dot(a, b, preferred_element_type=f32)


def hop(value, count, first, last, up):
    pairs = [(i, i + 1) for i in range(first, last)]
    if not up:
        pairs = [(count - 1 - a, count - 1 - b) for a, b in pairs]
    return lax.ppermute(value, "ra", pairs)


def line_reduce_scatter(parts, count):
    total = parts[0]
    up = down = None
    for step in range(count - 1):
        term = parts[count - 1 - step]
        up = hop((term if up is None else up.astype(f32) + term).astype(bf16), count, 0, min(step + 1, count - 1), True)
        term = parts[step + 1]
        down = hop((term if down is None else down.astype(f32) + term).astype(bf16), count, 0, min(step + 1, count - 1), False)
    return total + up.astype(f32) + down.astype(f32)


def line_all_gather(own, count):
    ups, downs = [], []
    up = down = own
    for step in range(count - 1):
        up = hop(up, count, step, count - 1, True)
        down = hop(down, count, step, count - 1, False)
        ups.append(up)
        downs.append(down)
    me = lax.axis_index("ra")
    return [own] + [
        jnp.where(me - 1 - step >= 0, ups[step], downs[count - 2 - step]) for step in range(count - 1)
    ]


def sum_small(value, count):
    total = value
    for shift in range(1, count):
        total = total + lax.ppermute(value, "ra", [(i, (i + shift) % count) for i in range(count)])
    return total


def sum_doubling(value, count):
    stride = 1
    while stride < count:
        other = lax.ppermute(value.astype(bf16), "cb", [(i, i ^ stride) for i in range(count)])
        value = value.astype(bf16).astype(f32) + other.astype(f32)
        stride *= 2
    return value


def shards(tokens, norm_gain, up_weight, up_scale, down_weight, down_scale):
    count, copies = lax.axis_size("ra"), lax.axis_size("cb")
    me = lax.axis_index("ra")
    block = up_weight.shape[2] // count
    chunks = max(1, 16 // count)
    size = tokens.shape[0] // chunks
    current = [tokens[k * size : (k + 1) * size] for k in range(chunks)]
    for layer in range(up_weight.shape[0]):
        ups, downs = [], []
        for j in range(count):
            owner = lax.rem(me + j, count)
            ups.append(lax.dynamic_slice_in_dim(up_weight[layer], owner * block, block, 1).astype(bf16))
            owner = lax.rem(me - j + count, count)
            downs.append(lax.dynamic_slice_in_dim(down_weight[layer], owner * block, block, 0).astype(bf16))
        ups, downs = lax.optimization_barrier((ups, downs))
        own_scale = lax.dynamic_slice_in_dim(up_scale[layer], me * block, block, 0)[None, :]
        results = []
        for k in range(chunks):
            widened = current[k].astype(f32)
            squares = sum_small(jnp.sum(widened * widened, axis=1), count)
            inverse = lax.rsqrt(squares / D + epsilon)[:, None]
            scaled = (widened * norm_gain[layer]).astype(bf16)
            upward = line_reduce_scatter([dot(scaled, w) for w in ups], count)
            active = jnp.maximum(upward * inverse * own_scale, 0.0)
            hidden = (active * active).astype(bf16)
            blocks = line_all_gather(hidden, count)
            downward = dot(blocks[0], downs[0])
            for piece, w in zip(blocks[1:], downs[1:]):
                downward = downward + dot(piece, w)
            summed = sum_doubling(downward, copies)
            results.append((residual_keep * widened + summed * down_scale[layer]).astype(bf16))
        current = results
    return jnp.concatenate(current, axis=0)


def solution(mesh):
    in_specs = (
        P("grp", "ra"),
        P(None, "ra"),
        P(None, "ra", "cb"),
        P(None, "cb"),
        P(None, "cb", "ra"),
        P(None, "ra"),
    )
    out_specs = P("grp", "ra")
    return jax.shard_map(shards, mesh=mesh, in_specs=in_specs, out_specs=out_specs, check_vma=False)
```

```python
import jax
import jax.numpy as jnp
from jax import lax
from jax.sharding import PartitionSpec as P

D = 4096


epsilon = 1e-06
residual_keep = 0.5


f32, bf16 = jnp.float32, jnp.bfloat16


def dot(a, b):
    return jnp.dot(a, b, preferred_element_type=f32)


def hop(value, count, first, last, up):
    pairs = [(i, i + 1) for i in range(first, last)]
    if not up:
        pairs = [(count - 1 - a, count - 1 - b) for a, b in pairs]
    return lax.ppermute(value, "ra", pairs)


def job(widened, ups, downs, gain, own_scale, down_scale, count, copies):
    me = lax.axis_index("ra")
    scaled = (widened * gain).astype(bf16)
    parts = [dot(scaled, w) for w in ups]
    squares = jnp.sum(widened * widened, axis=1)
    others = [
        lax.ppermute(squares, "ra", [(i, (i + shift) % count) for i in range(count)]) for shift in range(1, count)
    ]
    up, down = parts[count - 1].astype(bf16), parts[1].astype(bf16)
    parts, others, up, down = yield parts, others, up, down
    inverse = lax.rsqrt(sum(others, squares) / D + epsilon)[:, None]
    for step in range(count - 1):
        up = hop(up, count, 0, step + 1, True)
        down = hop(down, count, 0, step + 1, False)
        up, down = yield up, down
        if step < count - 2:
            up = (up.astype(f32) + parts[count - 2 - step]).astype(bf16)
            down = (down.astype(f32) + parts[step + 2]).astype(bf16)
    upward = parts[0] + up.astype(f32) + down.astype(f32)
    active = jnp.maximum(upward * inverse * own_scale, 0.0)
    hidden = (active * active).astype(bf16)
    uppers, lowers = [], []
    up = down = hidden
    for step in range(count - 1):
        up = hop(up, count, step, count - 1, True)
        down = hop(down, count, step, count - 1, False)
        up, down = yield up, down
        uppers.append(up)
        lowers.append(down)
    total = dot(hidden, downs[0])
    for step in range(count - 1):
        piece = jnp.where(me - 1 - step >= 0, uppers[step], lowers[count - 2 - step])
        total = total + dot(piece, downs[step + 1])
    total = yield total
    stride = 1
    while stride < copies:
        rounded = total.astype(bf16)
        other = lax.ppermute(rounded, "cb", [(i, i ^ stride) for i in range(copies)])
        rounded, other = yield rounded, other
        total = rounded.astype(f32) + other.astype(f32)
        stride *= 2
    return (residual_keep * widened + total * down_scale).astype(bf16)


def shards(tokens, norm_gain, up_weight, up_scale, down_weight, down_scale):
    count, copies = lax.axis_size("ra"), lax.axis_size("cb")
    me = lax.axis_index("ra")
    layers, block = up_weight.shape[0], up_weight.shape[2] // count
    chunks = max(1, 16 // count)
    size = tokens.shape[0] // chunks
    weights = []
    for layer in range(layers):
        ups, downs = [], []
        for j in range(count):
            owner = lax.rem(me + j, count)
            ups.append(lax.dynamic_slice_in_dim(up_weight[layer], owner * block, block, 1).astype(bf16))
            owner = lax.rem(me - j + count, count)
            downs.append(lax.dynamic_slice_in_dim(down_weight[layer], owner * block, block, 0).astype(bf16))
        own_scale = lax.dynamic_slice_in_dim(up_scale[layer], me * block, block, 0)[None, :]
        weights.append((lax.optimization_barrier(ups), lax.optimization_barrier(downs), own_scale))
    current = {(0, k): tokens[k * size : (k + 1) * size] for k in range(chunks)}
    waiting = [(layer, k) for layer in range(layers) for k in range(chunks)]
    running, slot = {}, 0
    while waiting or running:
        held = {}
        for name in list(running):
            make, value = running[name]
            try:
                held[name] = make.send(value)
            except StopIteration as stop:
                current[(name[0] + 1, name[1])] = stop.value
                del running[name]
        if waiting and slot >= count * (layers * chunks - len(waiting)) and waiting[0] in current:
            name = waiting.pop(0)
            ups, downs, own_scale = weights[name[0]]
            make = job(
                current[name].astype(f32), ups, downs, norm_gain[name[0]], own_scale, down_scale[name[0]], count, copies
            )
            running[name] = (make, None)
            held[name] = next(make)
        held = {str(name): value for name, value in held.items()}
        if held:
            held = lax.optimization_barrier(held)
        for name in running:
            running[name] = (running[name][0], held[str(name)])
        slot += 1
    return jnp.concatenate([current[(layers, k)] for k in range(chunks)], axis=0)


def solution(mesh):
    in_specs = (
        P("grp", "ra"),
        P(None, "ra"),
        P(None, "ra", "cb"),
        P(None, "cb"),
        P(None, "cb", "ra"),
        P(None, "ra"),
    )
    out_specs = P("grp", "ra")
    return jax.shard_map(shards, mesh=mesh, in_specs=in_specs, out_specs=out_specs, check_vma=False)
```
